32 devices in a mesh: sp: 16 (over z, y, x), tp: 2 (over core).
Axes of the slice: x: 2, y: 2, z: 4, core: 2. Of those that a mesh axis runs over, the one named last changes fastest.
Arguments:
- cotangent: bfloat16 [6144, 2048], P('sp'), may hold values from -6 to 6
- routes: int32 [6144, 2], P('sp'), may hold values from 0 to 15, all different within a row; in each aligned block of 384 rows (0 to 383, 384 to 767, ...) at most 72 rows name the same one
- route_weight: float32 [6144, 2], P('sp'), may hold values from 0.1 to 0.9
- expert_rows: bfloat16 [16, 1152, 2048], P('sp'), may hold values from -6 to 6
- gate_w: bfloat16 [16, 2048, 1024], P('sp', None, 'tp'), may hold values from -0.125 to 0.125
- up_w: bfloat16 [16, 2048, 1024], P('sp', None, 'tp'), may hold values from -0.125 to 0.125
- down_w: bfloat16 [16, 1024, 2048], P('sp', 'tp'), may hold values from -0.1875 to 0.1875
- in_x: bfloat16 [6144, 1024], P('sp', 'tp'), may hold values from -6 to 6
- in_y: bfloat16 [6144, 1024], P('sp', 'tp'), may hold values from -6 to 6
- state: bfloat16 [6144, 1024], P('sp', 'tp'), may hold values from -6 to 6
- conv_taps: float32 [4, 1024], P(None, 'tp'), may hold values from -3 to 3
- gate_a: bfloat16 [8, 128, 128], P('tp'), may hold values from -0.5 to 0.5
- gate_x: bfloat16 [8, 128, 128], P('tp'), may hold values from -0.5 to 0.5
- decay_rate: float32 [1024], P('tp'), as said below
- out_weight: bfloat16 [2048, 1024], P(None, 'tp'), may hold values from -0.1875 to 0.1875
Outputs:
- grad_gate: bfloat16 [16, 2048, 1024], P('sp', None, 'tp')
- grad_up: bfloat16 [16, 2048, 1024], P('sp', None, 'tp')
- grad_down: bfloat16 [16, 1024, 2048], P('sp', 'tp')
- grad_proj: float32 [2048, 1024], P('sp', 'tp')
- grad_x: float32 [6144, 1024], P('sp', 'tp')
- grad_y: float32 [6144, 1024], P('sp', 'tp')
The draws below stay inside these ranges and needn't reach their ends.
Inputs may be any that keep to these rules, and one draw needn't show every extreme that they name: `routes`: among the 768 pairs of one device's rows no expert appears more than 72 times, and some expert appears exactly 72 times; a row's two experts differ. `decay_rate`: positive.
All inputs are finite; a program needn't handle non-finite values.
Results may differ from the reference program's by a relative error of at most 0.0052.
The reference program's roundings to bfloat16 on the way count: a program that leaves them out, or rounds other values in their place, can miss the bound.
Values may be sent and summed in bfloat16 or wider, within the bound.
A program may use at most 128 MiB of HBM per device.

```python
import math
import jax
import jax.numpy as jnp
import numpy as np
from jax import lax

D = 2048
FF = 1024
BW = 1024
BLK = 128
TAPS = 4
TOK_DEV = 384
TOKENS = 6144
EXPERTS = 16
CAP = 72
ROWS_IN = 1152
FF_PART = 512
BLOCKS = 8
N_SP = 16
N_TP = 2


def draw_decay_rate(key, part):
    pick_key, slow_key, fast_key = jax.random.split(key, 3)
    slow_rate = jax.random.uniform(slow_key, (BW,), jnp.float32, 0.3, 1.0) * (2.3 / (4.0 * TOKENS))
    fast_rate = jax.random.uniform(fast_key, (BW,), jnp.float32, 0.0025, 0.0083)
    fast_share = 0.5
    is_fast = jax.random.uniform(pick_key, (BW,), jnp.float32) < fast_share
    return jnp.where(is_fast, fast_rate, slow_rate).astype(jnp.float32)


def strengthened(result, own_key, source, target, shards_of, factor):
    def block_of(dim):
        return (jnp.arange(result.shape[dim]) // (result.shape[dim] // shards_of)).reshape((-1,) + (1,) * (result.ndim - 1 - dim))

    near = jax.random.permutation(own_key, shards_of)[block_of(target)]
    second = (block_of(target) + shards_of // 2) % shards_of
    return jnp.where((block_of(source) == near) | (block_of(source) == second), factor * result, result)


def steps_of(own_key, dims, cuts, smallest, largest):
    loudness, own = 1.0, jax.random.fold_in(own_key, 6)
    for dim, parts in cuts:
        draws = jnp.exp(jax.random.uniform(jax.random.fold_in(own, dim), (parts,), jnp.float32, smallest / len(cuts), largest / len(cuts)))
        loudness = loudness * jnp.repeat(draws, dims[dim] // parts).reshape([-1 if axis == dim else 1 for axis in range(len(dims))])
    return loudness


def assign_block(key, own, number, rows, number_of, top, reach, lean):
    sequence = jax.random.permutation(key, number_of)
    heavy_load, usual = portions_of(number_of, rows * top, reach, lean, True), portions_of(number_of, rows * top, reach, lean, False)
    places = jnp.arange(number_of)

    def named(sizes, turn):
        used = int((sizes > 0).sum())
        fixed = max(1, used // 4)
        shifted = fixed + (places - fixed + turn * (used - fixed)) % max(1, number_of - fixed)
        return jnp.zeros((number_of,), jnp.int32).at[sequence[jnp.where(places < fixed, places, shifted)]].set(jnp.asarray(sizes, jnp.int32))

    sizes = jnp.where(number % 4 == 0, named(heavy_load, number // 4), named(usual, number - number // 4 - 1))
    mixed = jax.random.permutation(jax.random.fold_in(own, 3), number_of)
    giver, taker = mixed[0:number_of // 2 * 2:2], mixed[1:number_of // 2 * 2:2]
    slack = jnp.minimum(sizes[giver] - 1, reach - sizes[taker]) // 2
    slack = jnp.where((giver == sequence[0]) | (taker == sequence[0]) | (sizes[taker] == 0), 0, jnp.maximum(slack, 0))
    shifted = jax.random.randint(jax.random.fold_in(own, 4), (number_of // 2,), 0, 1 << 20) % (slack + 1)
    sizes = sizes.at[giver].add(-shifted).at[taker].add(shifted)
    labels = jnp.searchsorted(jnp.cumsum(sizes), jnp.arange(rows * top), side="right").astype(jnp.int32)
    table = labels.reshape(top, rows).T
    table = table[jax.random.permutation(jax.random.fold_in(own, 1), rows)]
    turn = jax.random.randint(jax.random.fold_in(own, 2), (rows, 1), 0, top)
    return jnp.take_along_axis(table, (jnp.arange(top)[None, :] + turn) % top, axis=1)


def portions_of(number_of, total, bound, lean, full):
    loads = [(1 << 20) // math.isqrt(rank ** lean) + 1 for rank in range(1, number_of + 1)]
    largest = bound if full else min(bound, max(-(-total // number_of), total * loads[0] // sum(loads)))
    least = 1 if total - largest >= number_of - 1 else 0
    given, rest = [largest] + [least] * (number_of - 1), total - largest - least * (number_of - 1)
    while rest > 0:
        candidates = [i for i in range(1, number_of) if given[i] < largest] or [i for i in range(1, number_of) if given[i] < bound]
        mass, left = sum([loads[i] for i in candidates]), rest
        for i in candidates:
            more = min(bound - given[i], max(1, left * loads[i] // mass), rest)
            given[i] = given[i] + more
            rest = rest - more
    return np.array(given)


def gaussian(stream_key, extent, deviation, most, shards=(), held_as=jnp.bfloat16):
    result = deviation * jax.random.normal(stream_key, extent, jnp.float32)
    if shards:
        result = result * steps_of(stream_key, extent, shards, -0.22, 0.18)
    return jnp.clip(result, -most, most).astype(held_as)


def noise_with(stream_key, shape, deviation, most, cuts, heavy, held_as=jnp.bfloat16):
    values = deviation * jax.random.normal(stream_key, shape, jnp.float32)
    if cuts:
        values = values * steps_of(stream_key, shape, cuts, -0.22, 0.18)
    return jnp.clip(strengthened(values, jax.random.fold_in(stream_key, 3), *heavy), -most, most).astype(held_as)


def setup_inputs(seed: int = 0) -> dict:
    key_list = jax.random.split(jax.random.key(seed), 16)
    cotangent = noise_with(key_list[0], (TOKENS, D), 1.0, 6.0, ((0, 16),), (0, 1, 16, 2.0))
    routes_keys = jax.random.split(jax.random.fold_in(key_list[1], 1), TOKENS // TOK_DEV)
    routes_turns = jax.random.permutation(jax.random.fold_in(key_list[1], 3), TOKENS // TOK_DEV)
    routes = jax.vmap(lambda own, number: assign_block(jax.random.fold_in(key_list[1], 2), own, number, TOK_DEV, EXPERTS, 2, CAP, 2))(routes_keys, routes_turns).reshape((TOKENS, 2))
    route_weight = jnp.clip(0.1 + 0.79999997 * jax.random.uniform(key_list[2], (TOKENS, 2), jnp.float32) ** steps_of(key_list[2], (TOKENS, 2), ((0, 16),), -0.2, 0.2), 0.1, 0.9)
    expert_rows = gaussian(key_list[3], (EXPERTS, ROWS_IN, D), 1.0, 6.0, ((0, 16),))
    gate_w = gaussian(key_list[4], (EXPERTS, D, FF), D ** -0.5, 0.125, ((0, 16), (2, 2)))
    up_w = gaussian(key_list[5], (EXPERTS, D, FF), D ** -0.5, 0.125, ((0, 16), (2, 2)))
    down_w = gaussian(key_list[6], (EXPERTS, FF, D), FF ** -0.5, 0.1875, ((0, 16), (1, 2)))
    in_x = gaussian(key_list[7], (TOKENS, BW), 1.0, 6.0, ((0, 16), (1, 2)))
    in_y = gaussian(key_list[8], (TOKENS, BW), 1.0, 6.0, ((0, 16), (1, 2)))
    state = gaussian(key_list[9], (TOKENS, BW), 1.0, 6.0, ((0, 16), (1, 2)))
    conv_taps = gaussian(key_list[10], (TAPS, BW), TAPS ** -0.5, 3.0, ((1, 2),), jnp.float32)
    gate_a = gaussian(key_list[11], (BLOCKS, BLK, BLK), BLK ** -0.5, 0.5, ((0, 2),))
    gate_x = gaussian(key_list[12], (BLOCKS, BLK, BLK), BLK ** -0.5, 0.5, ((0, 2),))
    decay_rate = draw_decay_rate(jax.random.fold_in(key_list[15], 71), 0)
    out_weight = gaussian(key_list[14], (D, BW), BW ** -0.5, 0.1875, ((1, 2),))
    return dict(cotangent=cotangent, routes=routes, route_weight=route_weight, expert_rows=expert_rows, gate_w=gate_w, up_w=up_w, down_w=down_w, in_x=in_x, in_y=in_y, state=state, conv_taps=conv_taps, gate_a=gate_a, gate_x=gate_x, decay_rate=decay_rate, out_weight=out_weight)


rate_scale = 8.0
floor_square = 0.01
inv_root_two = 0.7071067811865476
inv_root_tau = 0.3989422804014327

def linear_combine(earlier, later):
    return (earlier[0] * later[0], later[0] * earlier[1] + later[1])

def expert_backward(expert_item):
    saved_rows, upstream, weight_gate, weight_up, weight_down = expert_item
    pre_gate = jnp.dot(saved_rows, weight_gate, preferred_element_type=jnp.float32)
    pre_up = jnp.dot(saved_rows, weight_up, preferred_element_type=jnp.float32)
    gate_sigmoid = jax.nn.sigmoid(pre_gate)
    silu_value = pre_gate * gate_sigmoid
    active = (silu_value * pre_up).astype(jnp.bfloat16)
    grad_active = jnp.dot(upstream, weight_down.T, preferred_element_type=jnp.float32)
    grad_down = jnp.dot(active.T, upstream, preferred_element_type=jnp.float32).astype(jnp.bfloat16)
    up_adjoint = (grad_active * silu_value).astype(jnp.bfloat16)
    gate_adjoint = (grad_active * pre_up * gate_sigmoid * (1.0 + pre_gate * (1.0 - gate_sigmoid))).astype(jnp.bfloat16)
    grad_gate = jnp.dot(saved_rows.T, gate_adjoint, preferred_element_type=jnp.float32).astype(jnp.bfloat16)
    grad_up = jnp.dot(saved_rows.T, up_adjoint, preferred_element_type=jnp.float32).astype(jnp.bfloat16)
    total = jnp.zeros((saved_rows.shape[0], saved_rows.shape[1]), jnp.float32)
    for block_index in range(N_TP):
        lower = block_index * FF_PART
        piece = jnp.dot(gate_adjoint[:, lower:lower + FF_PART], weight_gate[:, lower:lower + FF_PART].T, preferred_element_type=jnp.float32)
        piece = piece + jnp.dot(up_adjoint[:, lower:lower + FF_PART], weight_up[:, lower:lower + FF_PART].T, preferred_element_type=jnp.float32)
        total = total + piece.astype(jnp.bfloat16).astype(jnp.float32)
    return (grad_gate, grad_up, grad_down, total.astype(jnp.bfloat16))

def reference(cotangent, routes, route_weight, expert_rows, gate_w, up_w, down_w, in_x, in_y, state, conv_taps, gate_a, gate_x, decay_rate, out_weight):
    pair_expert = routes.reshape(N_SP, TOK_DEV * 2)
    onehot = (pair_expert[:, :, None] == jnp.arange(EXPERTS, dtype=jnp.int32)[None, None, :]).astype(jnp.int32)
    before = (jnp.cumsum(onehot, axis=1) - onehot).astype(jnp.int32)
    position = lax.optimization_barrier(jnp.sum(before * onehot, axis=2)).astype(jnp.int32)
    source = jnp.arange(N_SP, dtype=jnp.int32)[:, None]
    target = (pair_expert * ROWS_IN + source * CAP + position).reshape(-1).astype(jnp.int32)
    token_ids = jnp.repeat(jnp.arange(TOKENS, dtype=jnp.int32), 2)
    slot_token = jnp.zeros((EXPERTS * ROWS_IN,), jnp.int32).at[target].set(token_ids)
    slot_weight = jnp.zeros((EXPERTS * ROWS_IN,), jnp.float32).at[target].set(route_weight.reshape(-1))
    upstream = (cotangent[slot_token].astype(jnp.float32) * slot_weight[:, None]).astype(jnp.bfloat16)
    upstream = upstream.reshape(EXPERTS, ROWS_IN, D)
    grad_gate, grad_up, grad_down, back_rows = lax.map(expert_backward, (expert_rows, upstream, gate_w, up_w, down_w))
    picked = back_rows.reshape(EXPERTS * ROWS_IN, D)[target].astype(jnp.float32).reshape(TOKENS, 2, D)
    stream_grad = (cotangent.astype(jnp.float32) + lax.optimization_barrier(jnp.sum(picked, axis=1))).astype(jnp.bfloat16)
    y_float = in_y.astype(jnp.float32)
    gelu_y = jax.nn.gelu(y_float, approximate=False)
    gelu_slope = 0.5 * (1.0 + lax.erf(y_float * inv_root_two)) + y_float * jnp.exp(-0.5 * y_float * y_float) * inv_root_tau
    state_float = state.astype(jnp.float32)
    mixed_out = (state_float * gelu_y).astype(jnp.bfloat16)
    grad_proj = jnp.dot(stream_grad.T, mixed_out, preferred_element_type=jnp.float32)
    grad_mixed = jnp.dot(stream_grad, out_weight, preferred_element_type=jnp.float32)
    grad_y = grad_mixed * state_float * gelu_slope
    grad_state = grad_mixed * gelu_y
    padded_x = jnp.concatenate([jnp.zeros((TAPS - 1, BW), jnp.float32), in_x.astype(jnp.float32)], axis=0)
    conv_x = conv_taps[0][None, :] * padded_x[0:TOKENS]
    for offset in range(1, TAPS):
        conv_x = conv_x + conv_taps[offset][None, :] * padded_x[offset:offset + TOKENS]
    conv_b = conv_x.astype(jnp.bfloat16).astype(jnp.float32).reshape(TOKENS, BLOCKS, BLK)
    keep_gate = jax.nn.sigmoid(jnp.einsum('tci,cij->tcj', conv_b, gate_a.astype(jnp.float32))).reshape(TOKENS, BW)
    input_gate = jax.nn.sigmoid(jnp.einsum('tci,cij->tcj', conv_b, gate_x.astype(jnp.float32))).reshape(TOKENS, BW)
    decay_step = jnp.exp(-rate_scale * keep_gate * decay_rate[None, :])
    norm_factor = jnp.sqrt(1.0 - decay_step * decay_step + floor_square)
    ahead_decay = jnp.concatenate([decay_step[1:], jnp.ones((1, BW), jnp.float32)], axis=0)
    scanned = lax.associative_scan(linear_combine, (ahead_decay[::-1], grad_state[::-1]), axis=0)
    adjoint = scanned[1][::-1]
    state_prev = jnp.concatenate([jnp.zeros((1, BW), jnp.float32), state_float[:-1]], axis=0)
    grad_norm = adjoint * conv_x * input_gate
    log_grad = adjoint * decay_step * state_prev - grad_norm * decay_step * decay_step / norm_factor
    keep_adjoint = (log_grad * (-rate_scale * decay_rate[None, :]) * keep_gate * (1.0 - keep_gate)).astype(jnp.bfloat16)
    input_adjoint = (adjoint * conv_x * norm_factor * input_gate * (1.0 - input_gate)).astype(jnp.bfloat16)
    back_keep = jnp.einsum('tcj,cij->tci', keep_adjoint.astype(jnp.float32).reshape(TOKENS, BLOCKS, BLK), gate_a.astype(jnp.float32))
    back_input = jnp.einsum('tcj,cij->tci', input_adjoint.astype(jnp.float32).reshape(TOKENS, BLOCKS, BLK), gate_x.astype(jnp.float32))
    conv_grad = adjoint * input_gate * norm_factor + back_keep.reshape(TOKENS, BW) + back_input.reshape(TOKENS, BW)
    padded_grad = jnp.concatenate([conv_grad, jnp.zeros((TAPS - 1, BW), jnp.float32)], axis=0)
    grad_x = conv_taps[0][None, :] * padded_grad[TAPS - 1:TAPS - 1 + TOKENS]
    for offset in range(1, TAPS):
        grad_x = grad_x + conv_taps[offset][None, :] * padded_grad[TAPS - 1 - offset:TAPS - 1 - offset + TOKENS]
    return (grad_gate, grad_up, grad_down, grad_proj, grad_x, grad_y)
```

```python
import functools

import jax
import jax.numpy as jnp
from jax import lax
from jax.experimental import pallas as pl
from jax.experimental.pallas import tpu as pltpu
from jax.sharding import PartitionSpec as P


rate_scale = 8.0
floor_square = 0.01
inv_root_two = 0.7071067811865476
inv_root_tau = 0.3989422804014327
lanes_of_rows = 8
MESH = pl.DeviceIdType.MESH


def shifted(value, axis, by):
    devices = lax.axis_size(axis)
    pairs = [(i, i + by) for i in range(devices) if 0 <= i + by < devices]
    return lax.ppermute(value, axis, pairs)


def from_other_core(value):
    return lax.ppermute(value, "tp", [(0, 1), (1, 0)])


def both_halves(mine):
    other = from_other_core(mine)
    first = lax.axis_index("tp") == 0
    return jnp.concatenate(
        [jnp.where(first, mine, other), jnp.where(first, other, mine)], axis=1
    )


def recurrence_kernel(
    count,
    grad_state,
    decay_step,
    conv_x,
    keep_gate,
    input_gate,
    state_prev,
    gate_a,
    gate_x,
    decay_rate,
    conv_taps,
    grad_x,
    local_adjoint,
    products,
    conv_grad,
    totals,
    halo,
    send_sem,
    recv_sem,
    halo_send,
    halo_recv,
):
    tokens, channels = grad_state.shape
    segments = lanes_of_rows
    assert tokens % segments == 0
    span = tokens // segments
    me = lax.axis_index("sp")
    barrier = pltpu.get_barrier_semaphore()
    for step in range(1, count):
        pl.semaphore_signal(
            barrier, inc=1, device_id={"sp": lax.rem(me + step, count)}, device_id_type=MESH
        )

    pieces, _, piece_width = local_adjoint.shape
    for piece in range(pieces):
        cols = slice(piece * piece_width, (piece + 1) * piece_width)
        local_adjoint[piece] = grad_state[:, cols]
        products[piece] = decay_step[:, cols]

    def scan_step(step, carry):
        rows = pl.ds(span - 1 - step, segments, stride=span)
        after = []
        for piece in range(pieces):
            product, carried = carry[piece]
            decay = products[piece, rows, :]
            adjoint = local_adjoint[piece, rows, :] + carried
            local_adjoint[piece, rows, :] = adjoint
            products[piece, rows, :] = product
            after.append((product * decay, decay * adjoint))
        return tuple(after)

    ends = lax.fori_loop(
        0,
        span,
        scan_step,
        tuple(
            (
                jnp.ones((segments, piece_width), jnp.float32),
                jnp.zeros((segments, piece_width), jnp.float32),
            )
            for _ in range(pieces)
        ),
        unroll=2,
    )
    product = jnp.concatenate([end[0] for end in ends], axis=1)
    carried = jnp.concatenate([end[1] for end in ends], axis=1)
    whole_product = jnp.ones((1, channels), jnp.float32)
    whole_carry = jnp.zeros((1, channels), jnp.float32)
    for segment in reversed(range(segments)):
        factor = product[segment : segment + 1]
        whole_carry = carried[segment : segment + 1] + factor * whole_carry
        whole_product = whole_product * factor
    totals[me, 0:1, :] = whole_product
    totals[me, 1:2, :] = whole_carry
    pl.semaphore_wait(barrier, count - 1)
    copies = []
    for step in range(1, count):
        copy = pltpu.make_async_remote_copy(
            src_ref=totals.at[me],
            dst_ref=totals.at[me],
            send_sem=send_sem.at[step],
            recv_sem=recv_sem.at[step],
            device_id={"sp": lax.rem(me + step, count)},
            device_id_type=MESH,
        )
        copy.start()
        copies.append(copy)
    for copy in copies:
        copy.wait()

    def join(step, carry_in):
        source = count - 1 - step
        longer = totals[source, 1:2, :] + totals[source, 0:1, :] * carry_in
        return jnp.where(source > me, longer, carry_in)

    carry_in = lax.fori_loop(0, count - 1, join, jnp.zeros((1, channels), jnp.float32))
    entering = [None] * segments
    for segment in reversed(range(segments)):
        entering[segment] = carry_in
        carry_in = carried[segment : segment + 1] + product[segment : segment + 1] * carry_in
    inner = (((1,), (1,)), ((), ()))
    block_span = gate_a.shape[1]
    for block in range(gate_a.shape[0]):
        lower = block * block_span
        upper = lower + block_span
        cols = slice(lower, upper)
        rate = -rate_scale * decay_rate[0:1, cols]
        weight_a = gate_a[block]
        weight_x = gate_x[block]
        for segment in range(segments):
            rows = slice(segment * span, (segment + 1) * span)
            adjoint = local_adjoint[block, rows, :] + products[block, rows, :] * entering[segment][:, cols]
            decay = decay_step[rows, cols]
            keep = keep_gate[rows, cols]
            gate = input_gate[rows, cols]
            conv = conv_x[rows, cols]
            norm = jnp.sqrt(1.0 - decay * decay + floor_square)
            grad_norm = adjoint * conv * gate
            log_grad = adjoint * decay * state_prev[rows, cols] - grad_norm * decay * decay / norm
            keep_adjoint = (log_grad * rate * keep * (1.0 - keep)).astype(jnp.bfloat16)
            input_adjoint = (adjoint * conv * norm * gate * (1.0 - gate)).astype(jnp.bfloat16)
            conv_grad[rows, cols] = (
                adjoint * gate * norm
                + lax.dot_general(keep_adjoint, weight_a, inner, preferred_element_type=jnp.float32)
                + lax.dot_general(
                    input_adjoint, weight_x, inner, preferred_element_type=jnp.float32
                )
            )
    edge = halo.shape[0]
    taps = conv_taps.shape[0]
    back = pltpu.make_async_remote_copy(
        src_ref=conv_grad.at[pl.ds(0, edge)],
        dst_ref=halo,
        send_sem=halo_send,
        recv_sem=halo_recv,
        device_id={"sp": lax.rem(me + count - 1, count)},
        device_id_type=MESH,
    )
    back.start()
    body_rows = tokens - edge
    for segment in range(segments):
        lower = segment * span
        upper = min(lower + span, body_rows)
        result = conv_taps[taps - 1 : taps, :] * conv_grad[lower:upper, :]
        for offset in range(1, taps):
            result = (
                result
                + conv_taps[taps - 1 - offset : taps - offset, :]
                * conv_grad[lower + offset : upper + offset, :]
            )
        grad_x[lower:upper, :] = result
    back.wait()
    conv_grad[tokens : tokens + edge, :] = jnp.where(me == count - 1, 0.0, halo[...])
    result = conv_taps[taps - 1 : taps, :] * conv_grad[body_rows:tokens, :]
    for offset in range(1, taps):
        result = (
            result
            + conv_taps[taps - 1 - offset : taps - offset, :]
            * conv_grad[body_rows + offset : tokens + offset, :]
        )
    grad_x[body_rows:tokens, :] = result


def recurrence(grad_state, decay_step, conv_x, keep_gate, input_gate, state_prev, gate_a, gate_x, decay_rate, conv_taps):
    count = lax.axis_size("sp")
    tokens, channels = grad_state.shape
    blocks = gate_a.shape[0]
    vmem = pl.BlockSpec(memory_space=pltpu.VMEM)
    return pl.pallas_call(
        functools.partial(recurrence_kernel, count),
        out_shape=jax.ShapeDtypeStruct((tokens, channels), jnp.float32),
        in_specs=[vmem] * 10,
        out_specs=vmem,
        scratch_shapes=[
            pltpu.VMEM((blocks, tokens, channels // blocks), jnp.float32),
            pltpu.VMEM((blocks, tokens, channels // blocks), jnp.float32),
            pltpu.VMEM((tokens + 8, channels), jnp.float32),
            pltpu.VMEM((count, 8, channels), jnp.float32),
            pltpu.VMEM((8, channels), jnp.float32),
            pltpu.SemaphoreType.DMA((count,)),
            pltpu.SemaphoreType.DMA((count,)),
            pltpu.SemaphoreType.DMA,
            pltpu.SemaphoreType.DMA,
        ],
        compiler_params=pltpu.CompilerParams(collective_id=1, has_side_effects=True),
        cost_estimate=pl.CostEstimate(
            flops=40 * tokens * channels, bytes_accessed=28 * tokens * channels, transcendentals=tokens * channels
        ),
        name="recurrence",
    )(grad_state, decay_step, conv_x, keep_gate, input_gate, state_prev, gate_a, gate_x, decay_rate[None, :], conv_taps)


def body(
    cotangent,
    routes,
    route_weight,
    expert_rows,
    gate_w,
    up_w,
    down_w,
    in_x,
    in_y,
    state,
    conv_taps,
    gate_a,
    gate_x,
    decay_rate,
    out_weight,
):
    tokens, model_width = cotangent.shape
    experts = lax.axis_size("sp")
    core_count = lax.axis_size("tp")
    core_index = lax.axis_index("tp")
    per_token = routes.shape[1]
    capacity = expert_rows.shape[1] // experts
    half_width = model_width // core_count
    slots = experts * capacity
    chosen = [
        (routes[:, k : k + 1] == jnp.arange(experts, dtype=jnp.int32)[None, :]) for k in range(per_token)
    ]
    named = functools.reduce(jnp.logical_or, chosen).astype(jnp.bfloat16)
    token_range = jnp.arange(tokens, dtype=jnp.int32)
    earlier = (token_range[None, :] < token_range[:, None]).astype(jnp.bfloat16)
    before = jnp.dot(earlier, named, preferred_element_type=jnp.float32).astype(jnp.int32)
    expert_range = jnp.arange(experts, dtype=jnp.int32)[None, :]
    slot_range = jnp.arange(slots, dtype=jnp.int32)
    select = jnp.zeros((slots, tokens), jnp.bool_)
    weighted = jnp.zeros((slots, tokens), jnp.float32)
    picker = jnp.zeros((tokens, slots), jnp.bool_)
    for k in range(per_token):
        place = jnp.sum(jnp.where(chosen[k], before + expert_range * capacity, 0), axis=1)
        hit = slot_range[:, None] == place[None, :]
        select = select | hit
        weighted = weighted + jnp.where(hit, route_weight[:, k][None, :], 0.0)
        picker = picker | (place[:, None] == slot_range[None, :])
    slot_weight = jnp.sum(weighted, axis=1)
    own_cols = lax.dynamic_slice_in_dim(cotangent, core_index * half_width, half_width, 1)
    outgoing = (
        jnp.dot(select.astype(jnp.bfloat16), own_cols, preferred_element_type=jnp.float32)
        * slot_weight[:, None]
    ).astype(jnp.bfloat16)
    arrived = lax.all_to_all(
        outgoing.reshape(experts, capacity, half_width),
        "sp",
        split_axis=0,
        concat_axis=0,
        tiled=True,
    )
    upstream = both_halves(arrived.reshape(-1, half_width))
    saved_rows = expert_rows[0]
    weight_gate = gate_w[0]
    weight_up = up_w[0]
    weight_down = down_w[0]
    pre_gate = jnp.dot(saved_rows, weight_gate, preferred_element_type=jnp.float32)
    pre_up = jnp.dot(saved_rows, weight_up, preferred_element_type=jnp.float32)
    gate_sigmoid = jax.nn.sigmoid(pre_gate)
    silu_value = pre_gate * gate_sigmoid
    active = (silu_value * pre_up).astype(jnp.bfloat16)
    inner = (((1,), (1,)), ((), ()))
    outer = (((0,), (0,)), ((), ()))
    grad_active = lax.dot_general(upstream, weight_down, inner, preferred_element_type=jnp.float32)
    grad_down = lax.dot_general(
        active, upstream, outer, preferred_element_type=jnp.float32
    ).astype(jnp.bfloat16)
    up_adjoint = (grad_active * silu_value).astype(jnp.bfloat16)
    gate_adjoint = (
        grad_active * pre_up * gate_sigmoid * (1.0 + pre_gate * (1.0 - gate_sigmoid))
    ).astype(jnp.bfloat16)
    grad_gate = lax.dot_general(
        saved_rows, gate_adjoint, outer, preferred_element_type=jnp.float32
    ).astype(jnp.bfloat16)
    grad_up = lax.dot_general(
        saved_rows, up_adjoint, outer, preferred_element_type=jnp.float32
    ).astype(jnp.bfloat16)

    def partial_of(core):
        rows_gate = lax.dynamic_slice_in_dim(weight_gate, core * half_width, half_width, 0)
        rows_up = lax.dynamic_slice_in_dim(weight_up, core * half_width, half_width, 0)
        value = lax.dot_general(gate_adjoint, rows_gate, inner, preferred_element_type=jnp.float32)
        value = value + lax.dot_general(
            up_adjoint, rows_up, inner, preferred_element_type=jnp.float32
        )
        return value.astype(jnp.bfloat16)

    arriving = from_other_core(partial_of(core_count - 1 - core_index))
    summed = partial_of(core_index).astype(jnp.float32) + arriving.astype(jnp.float32)
    returning = summed.astype(jnp.bfloat16).reshape(experts, capacity, half_width)
    returned = lax.all_to_all(returning, "sp", split_axis=0, concat_axis=0, tiled=True)
    picked = jnp.dot(
        picker.astype(jnp.bfloat16),
        returned.reshape(slots, half_width),
        preferred_element_type=jnp.float32,
    )
    stream_half = (own_cols.astype(jnp.float32) + picked).astype(jnp.bfloat16)
    stream = both_halves(stream_half)
    y_float = in_y.astype(jnp.float32)
    gelu_y = jax.nn.gelu(y_float, approximate=False)
    gelu_slope = (
        0.5 * (1.0 + lax.erf(y_float * inv_root_two))
        + y_float * jnp.exp(-0.5 * y_float * y_float) * inv_root_tau
    )
    state_float = state.astype(jnp.float32)
    early_y, early_state = lax.optimization_barrier((in_y, state))
    mixed_out = (
        early_state.astype(jnp.float32)
        * jax.nn.gelu(early_y.astype(jnp.float32), approximate=False)
    ).astype(jnp.bfloat16)
    proj_terms = lax.dot_general(
        stream, mixed_out, outer, preferred_element_type=jnp.float32
    ).astype(jnp.bfloat16)
    proj_terms = lax.all_to_all(
        proj_terms.reshape(experts, model_width // experts, -1),
        "sp",
        split_axis=0,
        concat_axis=0,
        tiled=True,
    )
    grad_proj = jnp.sum(proj_terms.astype(jnp.float32), axis=0)
    grad_mixed = jnp.dot(stream, out_weight, preferred_element_type=jnp.float32)
    grad_y = grad_mixed * state_float * gelu_slope
    grad_state = grad_mixed * gelu_y
    tap_count = conv_taps.shape[0]
    channels = in_x.shape[1]
    edge_rows = jnp.concatenate([in_x[tokens - tap_count + 1 :], state[tokens - 1 :]], axis=0)
    prior_rows = shifted(edge_rows, "sp", 1)
    extended = jnp.concatenate([prior_rows[: tap_count - 1], in_x], axis=0).astype(jnp.float32)
    state_prev = jnp.concatenate([prior_rows[tap_count - 1 :], state[:-1]], axis=0).astype(
        jnp.float32
    )
    conv_x = conv_taps[0][None, :] * extended[0:tokens]
    for offset in range(1, tap_count):
        conv_x = conv_x + conv_taps[offset][None, :] * extended[offset : offset + tokens]
    blocks = gate_a.shape[0]
    block_span = gate_a.shape[1]
    conv_b = conv_x.astype(jnp.bfloat16).reshape(tokens, blocks, block_span)
    keep_map = jnp.einsum("tci,cij->tcj", conv_b, gate_a, preferred_element_type=jnp.float32)
    input_map = jnp.einsum("tci,cij->tcj", conv_b, gate_x, preferred_element_type=jnp.float32)
    keep_gate = jax.nn.sigmoid(keep_map).reshape(tokens, channels)
    input_gate = jax.nn.sigmoid(input_map).reshape(tokens, channels)
    decay_step = jnp.exp(-rate_scale * keep_gate * decay_rate[None, :])
    grad_x = recurrence(
        grad_state, decay_step, conv_x, keep_gate, input_gate, state_prev, gate_a, gate_x, decay_rate, conv_taps
    )
    return (grad_gate[None], grad_up[None], grad_down[None], grad_proj, grad_x, grad_y)


def solution(mesh):
    in_specs = (
        P("sp", None),
        P("sp", None),
        P("sp", None),
        P("sp", None, None),
        P("sp", None, "tp"),
        P("sp", None, "tp"),
        P("sp", "tp", None),
        P("sp", "tp"),
        P("sp", "tp"),
        P("sp", "tp"),
        P(None, "tp"),
        P("tp", None, None),
        P("tp", None, None),
        P("tp"),
        P(None, "tp"),
    )
    out_specs = (
        P("sp", None, "tp"),
        P("sp", None, "tp"),
        P("sp", "tp", None),
        P("sp", "tp"),
        P("sp", "tp"),
        P("sp", "tp"),
    )
    return jax.shard_map(body, mesh=mesh, in_specs=in_specs, out_specs=out_specs, check_vma=False)
```
